32 devices in a mesh: ep: 8 (over z, x), tp: 4 (over y, core).
Axes of the slice: x: 2, y: 2, z: 4, core: 2. Of those that a mesh axis runs over, the one named last changes fastest.
Arguments:
- tokens: bfloat16 [1024, 2048], P('ep'), may hold values from -6 to 6
- norm_gain: float32 [2048], replicated, may hold values from 0.1 to 1.9
- expert_ids: int32 [1024, 2], P('ep'), may hold values from 0 to 7, all different within a row; in each aligned block of 128 rows (0 to 127, 128 to 255, ...) at most 64 rows name the same one
- route_weights: float32 [1024, 2], P('ep'), may hold values from 0.2 to 1
- w_gate: bfloat16 [8, 2048, 4096], P('ep', None, 'tp'), may hold values from -0.125 to 0.125
- w_up: bfloat16 [8, 2048, 4096], P('ep', None, 'tp'), may hold values from -0.125 to 0.125
- w_down: bfloat16 [8, 4096, 2048], P('ep', 'tp'), may hold values from -0.09375 to 0.09375
Outputs:
- combined: bfloat16 [1024, 2048], P('ep', 'tp')
The draws below stay inside these ranges and needn't reach their ends.
Inputs may be any that keep to these rules, and one draw needn't show every extreme that they name: `expert_ids`: each row names two different experts; among the rows of one device no expert is named more than 64 times, and in every draw some expert is named exactly 64 times there.
All inputs are finite; a program needn't handle non-finite values.
Results may differ from the reference program's by a relative error of at most 0.019.
Values may be sent and summed in bfloat16 or wider, within the bound.
A program may use at most 64 MiB of HBM per device.

```python
import math
import jax
import jax.numpy as jnp
import numpy as np
from jax import lax

D = 2048
FF = 4096
TOK_DEV = 128
EXPERTS = 8
CAP = 64
TOKENS = 1024
N_EP = 8
N_TP = 4


def block_scale(own_key, extent, pieces, low, top_value):
    loudness = 1.0
    for axis_at, blocks in pieces:
        draws = jax.random.uniform(jax.random.fold_in(jax.random.fold_in(own_key, 6), axis_at), (blocks,), jnp.float32, low / len(pieces), top_value / len(pieces))
        loudness = loudness * jnp.repeat(jnp.exp(draws), extent[axis_at] // blocks).reshape((-1,) + (1,) * (len(extent) - 1 - axis_at))
    return loudness


def routed_block(own_key, own, number, rows, count, top, bound, lean):
    sequence = jax.random.permutation(own_key, count)
    heavy_load, ordinary = shares(count, rows * top, bound, lean, True), shares(count, rows * top, bound, lean, False)
    places = jnp.arange(count)

    def named(sizes, turn):
        used = int((sizes > 0).sum())
        fixed = max(1, used // 4)
        passed = fixed + (places - fixed + turn * (used - fixed)) % max(1, count - fixed)
        return jnp.zeros((count,), jnp.int32).at[sequence[jnp.where(places < fixed, places, passed)]].set(jnp.asarray(sizes, jnp.int32))

    sizes = jnp.where(number % 4 == 0, named(heavy_load, number // 4), named(ordinary, number - number // 4 - 1))
    mixed = jax.random.permutation(jax.random.fold_in(own, 3), count)
    giver, sink = mixed[0:count // 2 * 2:2], mixed[1:count // 2 * 2:2]
    margin = jnp.minimum(sizes[giver] - 1, bound - sizes[sink]) // 2
    margin = jnp.where((giver == sequence[0]) | (sink == sequence[0]) | (sizes[sink] == 0), 0, jnp.maximum(margin, 0))
    passed = jax.random.randint(jax.random.fold_in(own, 4), (count // 2,), 0, 1 << 20) % (margin + 1)
    sizes = sizes.at[giver].add(-passed).at[sink].add(passed)
    items = jnp.searchsorted(jnp.cumsum(sizes), jnp.arange(rows * top), side="right").astype(jnp.int32)
    listing = items.reshape(top, rows).T
    listing = listing[jax.random.permutation(jax.random.fold_in(own, 1), rows)]
    turn = jax.random.randint(jax.random.fold_in(own, 2), (rows, 1), 0, top)
    return jnp.take_along_axis(listing, (jnp.arange(top)[None, :] + turn) % top, axis=1)


def shares(count, total, reach, slope, full):
    portions = [(1 << 20) // math.isqrt(rank ** slope) + 1 for rank in range(1, count + 1)]
    largest = reach if full else min(reach, max(-(-total // count), total * portions[0] // sum(portions)))
    least = 1 if total - largest >= count - 1 else 0
    counts, spare = [largest] + [least] * (count - 1), total - largest - least * (count - 1)
    while spare > 0:
        candidates = [i for i in range(1, count) if counts[i] < largest] or [i for i in range(1, count) if counts[i] < reach]
        mass, budget = sum([portions[i] for i in candidates]), spare
        for i in candidates:
            more = min(reach - counts[i], max(1, budget * portions[i] // mass), spare)
            counts[i] = counts[i] + more
            spare = spare - more
    return np.array(counts)


def centred(stream_key, extent, width, limit, shards=(), kind=jnp.bfloat16):
    result = width * jax.random.normal(stream_key, extent, jnp.float32)
    if shards:
        result = result * block_scale(stream_key, extent, shards, -0.22, 0.18)
    return jnp.clip(result, -limit, limit).astype(kind)


def setup_inputs(seed: int = 0) -> dict:
    seeds = jax.random.split(jax.random.key(seed), 8)
    tokens = centred(seeds[0], (TOKENS, D), 1.0, 6.0, ((0, 8),))
    norm_gain = jnp.clip(1.0 + 0.18 * jax.random.normal(seeds[1], (D,), jnp.float32), 0.1, 1.9)
    expert_ids_keys = jax.random.split(jax.random.fold_in(seeds[2], 1), TOKENS // TOK_DEV)
    expert_ids_turns = jax.random.permutation(jax.random.fold_in(seeds[2], 3), TOKENS // TOK_DEV)
    expert_ids = jax.vmap(lambda own, number: routed_block(jax.random.fold_in(seeds[2], 2), own, number, TOK_DEV, EXPERTS, 2, CAP, 2))(expert_ids_keys, expert_ids_turns).reshape((TOKENS, 2))
    route_weights = jnp.clip(0.2 + 0.8 * jax.random.uniform(seeds[3], (TOKENS, 2), jnp.float32) ** block_scale(seeds[3], (TOKENS, 2), ((0, 8),), -0.2, 0.2), 0.2, 1.0)
    w_gate = centred(seeds[4], (EXPERTS, D, FF), D ** -0.5, 0.125, ((0, 8), (2, 4)))
    w_up = centred(seeds[5], (EXPERTS, D, FF), D ** -0.5, 0.125, ((0, 8), (2, 4)))
    w_down = centred(seeds[6], (EXPERTS, FF, D), FF ** -0.5, 0.09375, ((0, 8), (1, 4)))
    return {"tokens": tokens, "norm_gain": norm_gain, "expert_ids": expert_ids, "route_weights": route_weights, "w_gate": w_gate, "w_up": w_up, "w_down": w_down}


epsilon = 1e-06

def run_expert(operands):
    rows, gate_weight, up_weight, down_weight = operands
    model_width = rows.shape[1]
    gate_values = jnp.dot(rows, gate_weight, preferred_element_type=jnp.float32)
    up_values = jnp.dot(rows, up_weight, preferred_element_type=jnp.float32)
    hidden = (jax.nn.silu(gate_values) * up_values).astype(jnp.bfloat16)
    grouped = hidden.reshape(rows.shape[0], N_TP, -1).astype(jnp.float32)
    down_groups = down_weight.reshape(N_TP, -1, model_width).astype(jnp.float32)
    partial_value = jnp.einsum('rtf,tfd->trd', grouped, down_groups)
    partial_value = lax.optimization_barrier(partial_value.astype(jnp.bfloat16)).astype(jnp.float32)
    return lax.optimization_barrier(jnp.sum(partial_value, axis=0)).astype(jnp.bfloat16)

def reference(tokens, norm_gain, expert_ids, route_weights, w_gate, w_up, w_down):
    model_width = tokens.shape[1]
    as_float = tokens.astype(jnp.float32)
    scale = lax.rsqrt(lax.optimization_barrier(jnp.mean(as_float * as_float, axis=-1, keepdims=True)) + epsilon)
    normed = (as_float * scale * norm_gain[None, :]).astype(jnp.bfloat16)
    flat_ids = expert_ids.reshape(N_EP, TOK_DEV * 2).astype(jnp.int32)
    one_hot = (flat_ids[:, :, None] == jnp.arange(EXPERTS, dtype=jnp.int32)[None, None, :]).astype(jnp.int32)
    slot_index = lax.optimization_barrier(jnp.sum((jnp.cumsum(one_hot, axis=1) - one_hot) * one_hot, axis=-1)).astype(jnp.int32)
    source = jnp.arange(N_EP, dtype=jnp.int32)[:, None]
    target = (flat_ids * (N_EP * CAP) + source * CAP + slot_index).reshape(-1).astype(jnp.int32)
    token_rows = jnp.repeat(normed, 2, axis=0)
    buffer = jnp.zeros((EXPERTS * N_EP * CAP, model_width), jnp.bfloat16).at[target].set(token_rows)
    buffer = buffer.reshape(EXPERTS, N_EP * CAP, model_width)
    expert_out = lax.map(run_expert, (buffer, w_gate, w_up, w_down))
    picked = expert_out.reshape(-1, model_width)[target].reshape(TOKENS, 2, model_width).astype(jnp.float32)
    return lax.optimization_barrier(jnp.sum(picked * route_weights[:, :, None], axis=1)).astype(jnp.bfloat16)
```

```python
import functools
import jax
import jax.numpy as jnp
from jax import lax
from jax.experimental import pallas as pl
from jax.experimental.pallas import tpu as pltpu
from jax.sharding import PartitionSpec as P

epsilon = 1e-06
MESH = pl.DeviceIdType.MESH
f32 = jnp.float32
bf16 = jnp.bfloat16


def kernel(n, tp, cap, tok_ref, gain_ref, ids_ref, rw_ref, wg_hbm, wu_hbm, wd_hbm, out_ref,
           wg, wu, wd, normed, send, xbuf, hid, part, rs1, s1, rs2, s2, ret, whi, wlo,
           w_sem, d_send, d_recv, y_send, y_recv, c_send, c_recv,
           p_send, p_recv, q_send, q_recv, r_send, r_recv):
    tok, width = tok_ref.shape
    ff = wg.shape[1]
    ny = tp // 2
    w = width // tp
    power = n & (n - 1) == 0
    half = n // 2
    me = lax.axis_index("ep")
    t = lax.axis_index("tp")
    core = lax.rem(t, 2)
    y = lax.div(t, 2)
    mate = y * 2 + 1 - core

    order = [0, 4, 1, 5, 2, 6, 3, 7] if n == 8 else None

    def shift(i, sign):
        if power:
            s = order[i] if order else i
            v, bit = me, 1
            while bit < n:
                if s & bit:
                    v = v + bit - 2 * bit * lax.rem(lax.div(v, bit), 2)
                bit *= 2
            return v
        return lax.rem(me + sign * i + n, n)

    def each(lo, hi, body):
        if power:
            for i in range(lo, hi):
                body(i)
        else:
            lax.fori_loop(lo, hi, lambda i, c: (body(i), c)[1], 0)

    def rows(i):
        return pl.ds(i * cap if isinstance(i, int) else pl.multiple_of(i * cap, cap), cap)

    def cols(p):
        return pl.ds(p * w if isinstance(p, int) else pl.multiple_of(p * w, w), w)

    def remote(src, dst, ss, rs, **where):
        return pltpu.make_async_remote_copy(
            src_ref=src, dst_ref=dst, send_sem=ss, recv_sem=rs,
            device_id=where, device_id_type=MESH)

    def y_peer(dy, sign=1):
        return lax.rem(y + sign * dy + ny, ny)

    def dispatch(i):
        e = shift(i, 1)
        return remote(send.at[rows(e)], xbuf.at[rows(i), cols(t)],
                      d_send.at[i], d_recv.at[i], ep=e)

    def y_copy(i, dy):
        at = xbuf.at[rows(i), cols(t)]
        return remote(at, at, y_send.at[i, dy], y_recv.at[i, dy], tp=y_peer(dy) * 2 + core)

    def y_wait(i, dy):
        at = xbuf.at[rows(i), cols(y_peer(dy, -1) * 2 + core)]
        remote(at, at, y_send.at[i, dy], y_recv.at[i, dy], tp=y_peer(dy) * 2 + core).wait_recv()

    def c_copy(i, dy):
        at = xbuf.at[rows(i), cols(y_peer(dy, -1) * 2 + core)]
        return remote(at, at, c_send.at[i, dy], c_recv.at[i, dy], tp=mate)

    def c_wait(i, dy):
        at = xbuf.at[rows(i), cols(y_peer(dy, -1) * 2 + 1 - core)]
        remote(at, at, c_send.at[i, dy], c_recv.at[i, dy], tp=mate).wait_recv()

    loads = [pltpu.make_async_copy(a.at[0], b, w_sem.at[k])
             for k, (a, b) in enumerate(((wg_hbm, wg), (wu_hbm, wu), (wd_hbm, wd)))]
    barrier = pltpu.get_barrier_semaphore()
    pl.semaphore_signal(barrier, inc=1, device_id={"tp": mate}, device_id_type=MESH)
    for dy in range(1, ny):
        pl.semaphore_signal(barrier, inc=1, device_id={"tp": y_peer(dy) * 2 + core},
                            device_id_type=MESH)
    each(1, n, lambda i: pl.semaphore_signal(
        barrier, inc=1, device_id={"ep": shift(i, 1)}, device_id_type=MESH))
    for load in loads:
        load.start()

    as_float = tok_ref[...].astype(f32)
    scale = lax.rsqrt(jnp.mean(as_float * as_float, axis=-1, keepdims=True) + epsilon)
    normed[...] = (as_float * scale * gain_ref[...]).astype(bf16)

    lanes = 128
    lane = lax.broadcasted_iota(jnp.int32, (tok, lanes), 1)
    first = ids_ref[:, 0:1] == lane
    second = ids_ref[:, 1:2] == lane
    named = (first | second).astype(f32).astype(bf16)
    weight = jnp.where(first, rw_ref[:, 0:1], 0.0) + jnp.where(second, rw_ref[:, 1:2], 0.0)
    earlier = (lax.broadcasted_iota(jnp.int32, (tok, tok), 1)
               < lax.broadcasted_iota(jnp.int32, (tok, tok), 0)).astype(f32).astype(bf16)
    before = jnp.dot(earlier, named, preferred_element_type=f32).astype(bf16)
    slots = n * cap
    j = lax.broadcasted_iota(jnp.int32, (lanes, slots), 1)
    spread = (lax.div(j, cap) == lax.broadcasted_iota(jnp.int32, (lanes, slots), 0))
    spread = spread.astype(f32).astype(bf16)
    at_slot = lax.rem(lax.broadcasted_iota(jnp.int32, (tok, slots), 1), cap).astype(f32)

    def spread_out(v):
        return jnp.dot(v, spread, preferred_element_type=f32)

    hit = jnp.where(spread_out(before) == at_slot, spread_out(named), 0.0)
    outgoing = lax.dot_general(hit.astype(bf16), normed[:, cols(t)],
                               (((0,), (0,)), ((), ())), preferred_element_type=f32)
    send[...] = outgoing.astype(bf16)

    pl.semaphore_wait(barrier, n - 1 + ny)
    each(1, n, lambda i: dispatch(i).start())

    mine = (lax.broadcasted_iota(jnp.int32, (lanes, cap), 0) == me).astype(f32).astype(bf16)
    own_slot = lax.broadcasted_iota(jnp.int32, (tok, cap), 1).astype(f32)
    own_hit = jnp.where(jnp.dot(before, mine, preferred_element_type=f32) == own_slot,
                        jnp.dot(named, mine, preferred_element_type=f32), 0.0)
    xbuf[0:cap, :] = lax.dot_general(own_hit.astype(bf16), normed[...],
                                     (((0,), (0,)), ((), ())),
                                     preferred_element_type=f32).astype(bf16)
    high = weight.astype(bf16)
    low = (weight - high.astype(f32)).astype(bf16)
    whi[...] = (hit * spread_out(high)).astype(bf16)
    wlo[...] = (hit * spread_out(low)).astype(bf16)

    def relay_first(lo, hi):
        def body(i):
            dispatch(i).wait_recv()
            for dy in range(1, ny):
                y_copy(i, dy).start()
            c_copy(i, 0).start()
        each(lo, hi, body)

    def relay_second(lo, hi):
        def body(i):
            for dy in range(1, ny):
                y_wait(i, dy)
                c_copy(i, dy).start()
        each(lo, hi, body)

    def settle(lo, hi):
        def body(i):
            for dy in range(ny):
                c_wait(i, dy)
        each(lo, hi, body)

    tile = min(256, ff)
    dtile = min(512, width)
    chunk = [pl.ds(0, half * cap), pl.ds(half * cap, (n - half) * cap)]

    def up(k):
        def step(f, c):
            at = pl.ds(pl.multiple_of(f * tile, tile), tile)
            x = xbuf[chunk[k], :]
            g = jnp.dot(x, wg[:, at], preferred_element_type=f32)
            u = jnp.dot(x, wu[:, at], preferred_element_type=f32)
            hid[chunk[k], at] = (g / (1.0 + jnp.exp(-g)) * u).astype(bf16)
            return c
        lax.fori_loop(0, ff // tile, step, 0)

    def down(k):
        def step(d, c):
            at = pl.ds(pl.multiple_of(d * dtile, dtile), dtile)
            part[chunk[k], at] = jnp.dot(hid[chunk[k], :], wd[:, at],
                                         preferred_element_type=f32).astype(bf16)
            return c
        lax.fori_loop(0, width // dtile, step, 0)

    def pair(k, v):
        return remote(part.at[chunk[k], cols(v * 2 + 1 - core)], rs1.at[chunk[k], cols(v)],
                      p_send.at[k, v], p_recv.at[k, v], tp=mate)

    def cross(k, dy):
        return remote(s1.at[chunk[k], cols(y_peer(dy))], rs2.at[dy - 1, chunk[k], :],
                      q_send.at[k, dy], q_recv.at[k, dy], tp=y_peer(dy) * 2 + core)

    def add_pair(k):
        for dy in [*range(1, ny), 0]:
            v = y_peer(dy)
            pair(k, v).wait_recv()
            s1[chunk[k], cols(v)] = (part[chunk[k], cols(v * 2 + core)].astype(f32)
                                     + rs1[chunk[k], cols(v)].astype(f32)).astype(bf16)
            if dy:
                cross(k, dy).start()

    def back(i):
        return remote(s2.at[rows(i)], ret.at[rows(me)], r_send.at[i], r_recv.at[i],
                      ep=shift(i, -1))

    def back_wait(i):
        e = shift(i, 1)
        remote(s2.at[rows(i)], ret.at[rows(e)], r_send.at[i], r_recv.at[i], ep=e).wait_recv()

    def add_cross(k):
        total = s1[chunk[k], cols(y)].astype(f32)
        for dy in range(1, ny):
            cross(k, dy).wait_recv()
            total = total + rs2[dy - 1, chunk[k], :].astype(f32)
        s2[chunk[k], :] = total.astype(bf16)
        if k == 0:
            each(1, half, lambda i: back(i).start())
            ret[rows(me), :] = s2[0:cap, :]
        else:
            each(half, n, lambda i: back(i).start())

    relay_first(1, half)
    relay_second(1, half)
    relay_first(half, n)
    settle(1, half)
    loads[0].wait()
    loads[1].wait()
    up(0)
    loads[2].wait()
    down(0)
    for v in range(ny):
        pair(0, v).start()
    relay_second(half, n)
    settle(half, n)
    add_pair(0)
    up(1)
    add_cross(0)
    down(1)
    for v in range(ny):
        pair(1, v).start()
    add_pair(1)
    add_cross(1)
    each(1, n, back_wait)
    out_ref[...] = (jnp.dot(whi[...], ret[...], preferred_element_type=f32)
                    + jnp.dot(wlo[...], ret[...], preferred_element_type=f32)).astype(bf16)

    def drain(i):
        dispatch(i).wait_send()
        for dy in range(1, ny):
            y_copy(i, dy).wait_send()
        for dy in range(ny):
            c_copy(i, dy).wait_send()
        back(i).wait_send()
    each(1, n, drain)
    for k in range(2):
        for v in range(ny):
            pair(k, v).wait_send()
        for dy in range(1, ny):
            cross(k, dy).wait_send()


def per_device(tokens, norm_gain, expert_ids, route_weights, w_gate, w_up, w_down):
    tok, width = tokens.shape
    n = lax.axis_size("ep")
    tp = lax.axis_size("tp")
    ff = w_gate.shape[2]
    experts = n * w_gate.shape[0]
    cap = -(-(4 * tok // experts) // 16) * 16
    w = width // tp
    ny = tp // 2
    r = n * cap
    dma = pltpu.SemaphoreType.DMA
    vmem = pl.BlockSpec(memory_space=pltpu.VMEM)
    anywhere = pl.BlockSpec(memory_space=pl.ANY)
    flops = 6 * r * width * ff
    return pl.pallas_call(
        functools.partial(kernel, n, tp, cap),
        out_shape=jax.ShapeDtypeStruct((tok, w), bf16),
        in_specs=[vmem] * 4 + [anywhere] * 3,
        out_specs=vmem,
        scratch_shapes=[
            pltpu.VMEM((width, ff), bf16),
            pltpu.VMEM((width, ff), bf16),
            pltpu.VMEM((ff, width), bf16),
            pltpu.VMEM((tok, width), bf16),
            pltpu.VMEM((r, w), bf16),
            pltpu.VMEM((r, width), bf16),
            pltpu.VMEM((r, ff), bf16),
            pltpu.VMEM((r, width), bf16),
            pltpu.VMEM((r, ny * w), bf16),
            pltpu.VMEM((r, ny * w), bf16),
            pltpu.VMEM((ny - 1, r, w), bf16),
            pltpu.VMEM((r, w), bf16),
            pltpu.VMEM((r, w), bf16),
            pltpu.VMEM((tok, r), bf16),
            pltpu.VMEM((tok, r), bf16),
            dma((3,)),
            dma((n,)), dma((n,)),
            dma((n, ny)), dma((n, ny)),
            dma((n, ny)), dma((n, ny)),
            dma((2, ny)), dma((2, ny)),
            dma((2, ny)), dma((2, ny)),
            dma((n,)), dma((n,)),
        ],
        compiler_params=pltpu.CompilerParams(
            collective_id=0, has_side_effects=True, vmem_limit_bytes=60 * 1024 * 1024),
        cost_estimate=pl.CostEstimate(
            flops=flops, bytes_accessed=6 * width * ff, transcendentals=r * ff),
    )(tokens, norm_gain.reshape(1, -1), expert_ids, route_weights, w_gate, w_up, w_down)


def solution(mesh):
    in_specs = (
        P("ep", None),
        P(),
        P("ep", None),
        P("ep", None),
        P("ep", None, "tp"),
        P("ep", None, "tp"),
        P("ep", "tp", None),
    )
    out_specs = P("ep", "tp")
    return jax.shard_map(
        per_device, mesh=mesh, in_specs=in_specs, out_specs=out_specs, check_vma=False
    )
```

```python
import functools
import jax
import jax.numpy as jnp
from jax import lax
from jax.experimental import pallas as pl
from jax.experimental.pallas import tpu as pltpu
from jax.sharding import PartitionSpec as P

epsilon = 1e-06
MESH = pl.DeviceIdType.MESH
f32 = jnp.float32
bf16 = jnp.bfloat16


def kernel(n, tp, cap, tok_ref, gain_ref, ids_ref, rw_ref, wg_hbm, wu_hbm, wd_hbm, out_ref,
           wg, wu, wd, normed, send, xbuf, hid, part, rs1, s1, rs2, s2, ret, whi, wlo,
           w_sem, d_send, d_recv, y_send, y_recv, c_send, c_recv,
           p_send, p_recv, q_send, q_recv, r_send, r_recv):
    tok, width = tok_ref.shape
    ff = wg.shape[1]
    ny = tp // 2
    w = width // tp
    power = n & (n - 1) == 0
    half = n // 2
    me = lax.axis_index("ep")
    t = lax.axis_index("tp")
    core = lax.rem(t, 2)
    y = lax.div(t, 2)
    mate = y * 2 + 1 - core

    order = [0, 1, 2, 4, 3, 5, 6, 7] if n == 8 else None

    def shift(i, sign):
        if power:
            s = order[i] if order else i
            v, bit = me, 1
            while bit < n:
                if s & bit:
                    v = v + bit - 2 * bit * lax.rem(lax.div(v, bit), 2)
                bit *= 2
            return v
        return lax.rem(me + sign * i + n, n)

    def each(lo, hi, body):
        if power:
            for i in range(lo, hi):
                body(i)
        else:
            lax.fori_loop(lo, hi, lambda i, c: (body(i), c)[1], 0)

    def rows(i):
        return pl.ds(i * cap if isinstance(i, int) else pl.multiple_of(i * cap, cap), cap)

    def cols(p):
        return pl.ds(p * w if isinstance(p, int) else pl.multiple_of(p * w, w), w)

    def remote(src, dst, ss, rs, **where):
        return pltpu.make_async_remote_copy(
            src_ref=src, dst_ref=dst, send_sem=ss, recv_sem=rs,
            device_id=where, device_id_type=MESH)

    def y_peer(dy, sign=1):
        return lax.rem(y + sign * dy + ny, ny)

    def dispatch(i):
        e = shift(i, 1)
        return remote(send.at[rows(e)], xbuf.at[rows(i), cols(t)],
                      d_send.at[i], d_recv.at[i], ep=e)

    def y_copy(i, dy):
        at = xbuf.at[rows(i), cols(t)]
        return remote(at, at, y_send.at[i, dy], y_recv.at[i, dy], tp=y_peer(dy) * 2 + core)

    def y_wait(i, dy):
        at = xbuf.at[rows(i), cols(y_peer(dy, -1) * 2 + core)]
        remote(at, at, y_send.at[i, dy], y_recv.at[i, dy], tp=y_peer(dy) * 2 + core).wait_recv()

    def c_copy(i, dy):
        at = xbuf.at[rows(i), cols(y_peer(dy, -1) * 2 + core)]
        return remote(at, at, c_send.at[i, dy], c_recv.at[i, dy], tp=mate)

    def c_wait(i, dy):
        at = xbuf.at[rows(i), cols(y_peer(dy, -1) * 2 + 1 - core)]
        remote(at, at, c_send.at[i, dy], c_recv.at[i, dy], tp=mate).wait_recv()

    loads = [pltpu.make_async_copy(a.at[0], b, w_sem.at[k])
             for k, (a, b) in enumerate(((wg_hbm, wg), (wu_hbm, wu), (wd_hbm, wd)))]
    barrier = pltpu.get_barrier_semaphore()
    pl.semaphore_signal(barrier, inc=1, device_id={"tp": mate}, device_id_type=MESH)
    for dy in range(1, ny):
        pl.semaphore_signal(barrier, inc=1, device_id={"tp": y_peer(dy) * 2 + core},
                            device_id_type=MESH)
    each(1, n, lambda i: pl.semaphore_signal(
        barrier, inc=1, device_id={"ep": shift(i, 1)}, device_id_type=MESH))
    for load in loads:
        load.start()

    as_float = tok_ref[...].astype(f32)
    scale = lax.rsqrt(jnp.mean(as_float * as_float, axis=-1, keepdims=True) + epsilon)
    normed[...] = (as_float * scale * gain_ref[...]).astype(bf16)

    slots = n * cap
    experts = 128
    first, second = ids_ref[0:1, :], ids_ref[1:2, :]
    expert = lax.broadcasted_iota(jnp.int32, (experts, tok), 0)
    is_first, is_second = first == expert, second == expert
    named = (is_first | is_second).astype(f32).astype(bf16)
    earlier = (lax.broadcasted_iota(jnp.int32, (tok, tok), 0)
               < lax.broadcasted_iota(jnp.int32, (tok, tok), 1)).astype(f32).astype(bf16)
    before = jnp.dot(named, earlier, preferred_element_type=f32)
    place1 = first * cap + jnp.sum(jnp.where(is_first, before, 0.0), axis=0,
                                   keepdims=True).astype(jnp.int32)
    place2 = second * cap + jnp.sum(jnp.where(is_second, before, 0.0), axis=0,
                                    keepdims=True).astype(jnp.int32)
    slot = lax.broadcasted_iota(jnp.int32, (slots, tok), 0)
    hit1, hit2 = slot == place1, slot == place2
    send[...] = jnp.dot((hit1 | hit2).astype(f32).astype(bf16), normed[:, cols(t)],
                        preferred_element_type=f32).astype(bf16)

    pl.semaphore_wait(barrier, n - 1 + ny)
    each(1, n, lambda i: dispatch(i).start())

    own = lax.broadcasted_iota(jnp.int32, (cap, tok), 0) + me * cap
    own_hit = ((own == place1) | (own == place2)).astype(f32).astype(bf16)
    xbuf[0:cap, :] = jnp.dot(own_hit, normed[...], preferred_element_type=f32).astype(bf16)
    weight = (jnp.where(hit1, rw_ref[0:1, :], 0.0) + jnp.where(hit2, rw_ref[1:2, :], 0.0)).T
    high = weight.astype(bf16)
    whi[...] = high
    wlo[...] = (weight - high.astype(f32)).astype(bf16)

    def relay_first(lo, hi):
        def body(i):
            dispatch(i).wait_recv()
            for dy in range(1, ny):
                y_copy(i, dy).start()
            c_copy(i, 0).start()
        each(lo, hi, body)

    def relay_second(lo, hi):
        def body(i):
            for dy in range(1, ny):
                y_wait(i, dy)
                c_copy(i, dy).start()
        each(lo, hi, body)

    def settle(lo, hi):
        def body(i):
            for dy in range(ny):
                c_wait(i, dy)
        each(lo, hi, body)

    tile = min(256, ff)
    chunk = [pl.ds(0, half * cap), pl.ds(half * cap, (n - half) * cap)]

    def up(k, lo, hi):
        def step(f, c):
            at = pl.ds(pl.multiple_of(f * tile, tile), tile)
            x = xbuf[chunk[k], :]
            g = jnp.dot(x, wg[:, at], preferred_element_type=f32)
            u = jnp.dot(x, wu[:, at], preferred_element_type=f32)
            hid[chunk[k], at] = (g / (1.0 + jnp.exp(-g)) * u).astype(bf16)
            return c
        lax.fori_loop(lo, hi, step, 0)

    def down(k, c):
        def step(v, carry):
            at = cols(v * 2 + c)
            part[chunk[k], at] = jnp.dot(hid[chunk[k], :], wd[:, at],
                                         preferred_element_type=f32).astype(bf16)
            return carry
        lax.fori_loop(0, ny, step, 0)

    def pair(k, v):
        return remote(part.at[chunk[k], cols(v * 2 + 1 - core)], rs1.at[chunk[k], cols(v)],
                      p_send.at[k, v], p_recv.at[k, v], tp=mate)

    def cross(i, dy):
        return remote(s1.at[rows(i), cols(y_peer(dy))], rs2.at[dy - 1, rows(i), :],
                      q_send.at[i, dy], q_recv.at[i, dy], tp=y_peer(dy) * 2 + core)

    def add_pair(k):
        for dy in [*range(1, ny), 0]:
            v = y_peer(dy)
            pair(k, v).wait_recv()
            s1[chunk[k], cols(v)] = (part[chunk[k], cols(v * 2 + core)].astype(f32)
                                     + rs1[chunk[k], cols(v)].astype(f32)).astype(bf16)
            if dy:
                each(*span[k], lambda i: cross(i, dy).start())

    def back(i):
        return remote(s2.at[rows(i)], ret.at[rows(me)], r_send.at[i], r_recv.at[i],
                      ep=shift(i, -1))

    def back_wait(i):
        e = shift(i, 1)
        remote(s2.at[rows(i)], ret.at[rows(e)], r_send.at[i], r_recv.at[i], ep=e).wait_recv()

    def total(i):
        value = s1[rows(i), cols(y)].astype(f32)
        for dy in range(1, ny):
            cross(i, dy).wait_recv()
            value = value + rs2[dy - 1, rows(i), :].astype(f32)
        return value.astype(bf16)

    def finish(lo, hi):
        def body(i):
            s2[rows(i), :] = total(i)
            back(i).start()
        each(lo, hi, body)

    span = [(0, half), (half, n)]
    tiles = ff // tile
    relay_first(1, n)
    relay_second(1, half)
    settle(1, half)
    loads[0].wait()
    loads[1].wait()
    up(0, 0, tiles)
    relay_second(half, n)
    loads[2].wait()
    down(0, 1 - core)
    for v in range(ny):
        pair(0, v).start()
    down(0, core)
    settle(half, n)
    up(1, 0, tiles // 2)
    add_pair(0)
    up(1, tiles // 2, tiles)
    finish(1, 2)
    down(1, 1 - core)
    for v in range(ny):
        pair(1, v).start()
    finish(2, half)
    down(1, core)
    add_pair(1)
    ret[rows(me), :] = total(0)
    finish(half, n)
    each(1, n, back_wait)
    out_ref[...] = (jnp.dot(whi[...], ret[...], preferred_element_type=f32)
                    + jnp.dot(wlo[...], ret[...], preferred_element_type=f32)).astype(bf16)

    def drain(i):
        dispatch(i).wait_send()
        for dy in range(1, ny):
            y_copy(i, dy).wait_send()
        for dy in range(ny):
            c_copy(i, dy).wait_send()
        back(i).wait_send()
    each(1, n, drain)

    def drain_cross(i):
        for dy in range(1, ny):
            cross(i, dy).wait_send()
    each(0, n, drain_cross)
    for k in range(2):
        for v in range(ny):
            pair(k, v).wait_send()


def per_device(tokens, norm_gain, expert_ids, route_weights, w_gate, w_up, w_down):
    tok, width = tokens.shape
    n = lax.axis_size("ep")
    tp = lax.axis_size("tp")
    ff = w_gate.shape[2]
    experts = n * w_gate.shape[0]
    cap = -(-(4 * tok // experts) // 16) * 16
    w = width // tp
    ny = tp // 2
    r = n * cap
    dma = pltpu.SemaphoreType.DMA
    vmem = pl.BlockSpec(memory_space=pltpu.VMEM)
    anywhere = pl.BlockSpec(memory_space=pl.ANY)
    flops = 6 * r * width * ff
    return pl.pallas_call(
        functools.partial(kernel, n, tp, cap),
        out_shape=jax.ShapeDtypeStruct((tok, w), bf16),
        in_specs=[vmem] * 4 + [anywhere] * 3,
        out_specs=vmem,
        scratch_shapes=[
            pltpu.VMEM((width, ff), bf16),
            pltpu.VMEM((width, ff), bf16),
            pltpu.VMEM((ff, width), bf16),
            pltpu.VMEM((tok, width), bf16),
            pltpu.VMEM((r, w), bf16),
            pltpu.VMEM((r, width), bf16),
            pltpu.VMEM((r, ff), bf16),
            pltpu.VMEM((r, width), bf16),
            pltpu.VMEM((r, ny * w), bf16),
            pltpu.VMEM((r, ny * w), bf16),
            pltpu.VMEM((ny - 1, r, w), bf16),
            pltpu.VMEM((r, w), bf16),
            pltpu.VMEM((r, w), bf16),
            pltpu.VMEM((tok, r), bf16),
            pltpu.VMEM((tok, r), bf16),
            dma((3,)),
            dma((n,)), dma((n,)),
            dma((n, ny)), dma((n, ny)),
            dma((n, ny)), dma((n, ny)),
            dma((2, ny)), dma((2, ny)),
            dma((n, ny)), dma((n, ny)),
            dma((n,)), dma((n,)),
        ],
        compiler_params=pltpu.CompilerParams(
            collective_id=0, has_side_effects=True, vmem_limit_bytes=60 * 1024 * 1024),
        cost_estimate=pl.CostEstimate(
            flops=flops, bytes_accessed=6 * width * ff, transcendentals=r * ff),
    )(tokens, norm_gain.reshape(1, -1), expert_ids.T, route_weights.T, w_gate, w_up, w_down)


def solution(mesh):
    in_specs = (
        P("ep", None),
        P(),
        P("ep", None),
        P("ep", None),
        P("ep", None, "tp"),
        P("ep", None, "tp"),
        P("ep", "tp", None),
    )
    out_specs = P("ep", "tp")
    return jax.shard_map(
        per_device, mesh=mesh, in_specs=in_specs, out_specs=out_specs, check_vma=False
    )
```

```python
import functools
import jax
import jax.numpy as jnp
from jax import lax
from jax.experimental import pallas as pl
from jax.experimental.pallas import tpu as pltpu
from jax.sharding import PartitionSpec as P

epsilon = 1e-06
MESH = pl.DeviceIdType.MESH
f32 = jnp.float32
bf16 = jnp.bfloat16


def kernel(n, tp, cap, tok_ref, gain_ref, ids_ref, rw_ref, wg_hbm, wu_hbm, wd_hbm, out_ref,
           wg, wu, wd, normed, send, send2, xbuf, hid, part, rs1, s1, rs2, s2, ret, whi, wlo,
           w_sem, d_send, d_recv, y_send, y_recv, c_send, c_recv,
           p_send, p_recv, q_send, q_recv, r_send, r_recv):
    tok, width = tok_ref.shape
    ff = wg.shape[1]
    ny = tp // 2
    w = width // tp
    power = n & (n - 1) == 0
    half = n // 2
    me = lax.axis_index("ep")
    t = lax.axis_index("tp")
    core = lax.rem(t, 2)
    y = lax.div(t, 2)
    mate = y * 2 + 1 - core

    order = [0, 1, 4, 5, 2, 3, 6, 7] if n == 8 else None
    direct = [1, 4] if n == 8 and ny == 2 else []
    cross_order = [[2, 3, 1, 0], [6, 7, 5, 4]] if n == 8 else None

    def shift(i, sign):
        if power:
            s = order[i] if order else i
            v, bit = me, 1
            while bit < n:
                if s & bit:
                    v = v + bit - 2 * bit * lax.rem(lax.div(v, bit), 2)
                bit *= 2
            return v
        return lax.rem(me + sign * i + n, n)

    def each(lo, hi, body):
        if power:
            for i in range(lo, hi):
                body(i)
        else:
            lax.fori_loop(lo, hi, lambda i, c: (body(i), c)[1], 0)

    def rows(i):
        return pl.ds(i * cap if isinstance(i, int) else pl.multiple_of(i * cap, cap), cap)

    def cols(p):
        return pl.ds(p * w if isinstance(p, int) else pl.multiple_of(p * w, w), w)

    def remote(src, dst, ss, rs, **where):
        return pltpu.make_async_remote_copy(
            src_ref=src, dst_ref=dst, send_sem=ss, recv_sem=rs,
            device_id=where, device_id_type=MESH)

    def y_peer(dy, sign=1):
        return lax.rem(y + sign * dy + ny, ny)

    def dispatch(i):
        e = shift(i, 1)
        return remote(send.at[rows(e)], xbuf.at[rows(i), cols(t)],
                      d_send.at[i], d_recv.at[i], ep=e)

    def y_copy(i, dy):
        at = xbuf.at[rows(i), cols(t)]
        return remote(at, at, y_send.at[i, dy], y_recv.at[i, dy], tp=y_peer(dy) * 2 + core)

    def y_wait(i, dy):
        at = xbuf.at[rows(i), cols(y_peer(dy, -1) * 2 + core)]
        remote(at, at, y_send.at[i, dy], y_recv.at[i, dy], tp=y_peer(dy) * 2 + core).wait_recv()

    def c_copy(i, dy):
        at = xbuf.at[rows(i), cols(y_peer(dy, -1) * 2 + core)]
        return remote(at, at, c_send.at[i, dy], c_recv.at[i, dy], tp=mate)

    def c_wait(i, dy):
        at = xbuf.at[rows(i), cols(y_peer(dy, -1) * 2 + 1 - core)]
        remote(at, at, c_send.at[i, dy], c_recv.at[i, dy], tp=mate).wait_recv()

    loads = [pltpu.make_async_copy(a.at[0], b, w_sem.at[k])
             for k, (a, b) in enumerate(((wg_hbm, wg), (wu_hbm, wu), (wd_hbm, wd)))]
    barrier = pltpu.get_barrier_semaphore()
    pl.semaphore_signal(barrier, inc=1, device_id={"tp": mate}, device_id_type=MESH)
    for dy in range(1, ny):
        pl.semaphore_signal(barrier, inc=1, device_id={"tp": y_peer(dy) * 2 + core},
                            device_id_type=MESH)
    each(1, n, lambda i: pl.semaphore_signal(
        barrier, inc=1, device_id={"ep": shift(i, 1)}, device_id_type=MESH))
    for load in loads:
        load.start()

    as_float = tok_ref[...].astype(f32)
    scale = lax.rsqrt(jnp.mean(as_float * as_float, axis=-1, keepdims=True) + epsilon)
    normed[...] = (as_float * scale * gain_ref[...]).astype(bf16)

    slots = n * cap
    experts = 128
    first, second = ids_ref[0:1, :], ids_ref[1:2, :]
    expert = lax.broadcasted_iota(jnp.int32, (experts, tok), 0)
    is_first, is_second = first == expert, second == expert
    named = (is_first | is_second).astype(f32).astype(bf16)
    earlier = (lax.broadcasted_iota(jnp.int32, (tok, tok), 0)
               < lax.broadcasted_iota(jnp.int32, (tok, tok), 1)).astype(f32).astype(bf16)
    before = jnp.dot(named, earlier, preferred_element_type=f32)
    place1 = first * cap + jnp.sum(jnp.where(is_first, before, 0.0), axis=0,
                                   keepdims=True).astype(jnp.int32)
    place2 = second * cap + jnp.sum(jnp.where(is_second, before, 0.0), axis=0,
                                    keepdims=True).astype(jnp.int32)
    slot = lax.broadcasted_iota(jnp.int32, (slots, tok), 0)
    hit1, hit2 = slot == place1, slot == place2
    send[...] = jnp.dot((hit1 | hit2).astype(f32).astype(bf16), normed[:, cols(t)],
                        preferred_element_type=f32).astype(bf16)

    pl.semaphore_wait(barrier, n - 1 + ny)
    each(1, n, lambda i: dispatch(i).start())

    for i in direct:
        e = shift(i, 1)
        row = lax.broadcasted_iota(jnp.int32, (cap, tok), 0) + e * cap
        at_row = ((row == place1) | (row == place2)).astype(f32).astype(bf16)
        other = cols(y_peer(1) * 2 + core)
        send2[rows(i), :] = jnp.dot(at_row, normed[:, other],
                                    preferred_element_type=f32).astype(bf16)
        remote(send2.at[rows(i)], xbuf.at[rows(i), other],
               y_send.at[i, 1], y_recv.at[i, 1], ep=e).start()

    own = lax.broadcasted_iota(jnp.int32, (cap, tok), 0) + me * cap
    own_hit = ((own == place1) | (own == place2)).astype(f32).astype(bf16)
    xbuf[0:cap, :] = jnp.dot(own_hit, normed[...], preferred_element_type=f32).astype(bf16)
    weight = (jnp.where(hit1, rw_ref[0:1, :], 0.0) + jnp.where(hit2, rw_ref[1:2, :], 0.0)).T
    high = weight.astype(bf16)
    whi[...] = high
    wlo[...] = (weight - high.astype(f32)).astype(bf16)

    def relay_first(lo, hi):
        def body(i):
            dispatch(i).wait_recv()
            for dy in range(1, ny):
                if i not in direct:
                    y_copy(i, dy).start()
            c_copy(i, 0).start()
        each(lo, hi, body)

    def relay_second(lo, hi):
        def body(i):
            for dy in range(1, ny):
                y_wait(i, dy)
                c_copy(i, dy).start()
        each(lo, hi, body)

    def settle(lo, hi):
        def body(i):
            for dy in range(ny):
                c_wait(i, dy)
        each(lo, hi, body)

    tile = min(256, ff)
    chunk = [pl.ds(0, half * cap), pl.ds(half * cap, (n - half) * cap)]

    def up(k, lo, hi):
        def step(f, c):
            at = pl.ds(pl.multiple_of(f * tile, tile), tile)
            x = xbuf[chunk[k], :]
            g = jnp.dot(x, wg[:, at], preferred_element_type=f32)
            u = jnp.dot(x, wu[:, at], preferred_element_type=f32)
            hid[chunk[k], at] = (g / (1.0 + jnp.exp(-g)) * u).astype(bf16)
            return c
        lax.fori_loop(lo, hi, step, 0)

    def down(k, c):
        def step(v, carry):
            at = cols(v * 2 + c)
            part[chunk[k], at] = jnp.dot(hid[chunk[k], :], wd[:, at],
                                         preferred_element_type=f32).astype(bf16)
            return carry
        lax.fori_loop(0, ny, step, 0)

    def pair(k, v):
        return remote(part.at[chunk[k], cols(v * 2 + 1 - core)], rs1.at[chunk[k], cols(v)],
                      p_send.at[k, v], p_recv.at[k, v], tp=mate)

    def cross(i, dy):
        return remote(s1.at[rows(i), cols(y_peer(dy))], rs2.at[dy - 1, rows(i), :],
                      q_send.at[i, dy], q_recv.at[i, dy], tp=y_peer(dy) * 2 + core)

    def add_pair(k):
        for dy in [*range(1, ny), 0]:
            v = y_peer(dy)
            pair(k, v).wait_recv()
            s1[chunk[k], cols(v)] = (part[chunk[k], cols(v * 2 + core)].astype(f32)
                                     + rs1[chunk[k], cols(v)].astype(f32)).astype(bf16)
            if dy:
                if cross_order:
                    for i in cross_order[k]:
                        cross(i, dy).start()
                else:
                    each(*span[k], lambda i: cross(i, dy).start())

    def back(i):
        return remote(s2.at[rows(i)], ret.at[rows(me)], r_send.at[i], r_recv.at[i],
                      ep=shift(i, -1))

    def back_wait(i):
        e = shift(i, 1)
        remote(s2.at[rows(i)], ret.at[rows(e)], r_send.at[i], r_recv.at[i], ep=e).wait_recv()

    def total(i):
        value = s1[rows(i), cols(y)].astype(f32)
        for dy in range(1, ny):
            cross(i, dy).wait_recv()
            value = value + rs2[dy - 1, rows(i), :].astype(f32)
        return value.astype(bf16)

    def finish(k, lo, hi):
        def body(i):
            s2[rows(i), :] = total(i)
            back(i).start()
        if cross_order:
            for i in [i for i in cross_order[k] if i][lo - k * half - (k == 0):hi - k * half - (k == 0)]:
                body(i)
        else:
            each(lo, hi, body)

    span = [(0, half), (half, n)]
    tiles = ff // tile
    relay_first(1, n)
    relay_second(1, half)
    settle(1, half)
    loads[0].wait()
    loads[1].wait()
    up(0, 0, tiles)
    relay_second(half, n)
    loads[2].wait()
    down(0, 1 - core)
    for v in range(ny):
        pair(0, v).start()
    down(0, core)
    add_pair(0)
    settle(half, n)
    up(1, 0, tiles)
    finish(0, 1, 2)
    down(1, 1 - core)
    for v in range(ny):
        pair(1, v).start()
    finish(0, 2, half)
    down(1, core)
    add_pair(1)
    ret[rows(me), :] = total(0)
    finish(1, half, n)
    each(1, n, back_wait)
    out_ref[...] = (jnp.dot(whi[...], ret[...], preferred_element_type=f32)
                    + jnp.dot(wlo[...], ret[...], preferred_element_type=f32)).astype(bf16)

    def drain(i):
        dispatch(i).wait_send()
        for dy in range(1, ny):
            y_copy(i, dy).wait_send()
        for dy in range(ny):
            c_copy(i, dy).wait_send()
        back(i).wait_send()
    each(1, n, drain)

    def drain_cross(i):
        for dy in range(1, ny):
            cross(i, dy).wait_send()
    each(0, n, drain_cross)
    for k in range(2):
        for v in range(ny):
            pair(k, v).wait_send()


def per_device(tokens, norm_gain, expert_ids, route_weights, w_gate, w_up, w_down):
    tok, width = tokens.shape
    n = lax.axis_size("ep")
    tp = lax.axis_size("tp")
    ff = w_gate.shape[2]
    experts = n * w_gate.shape[0]
    cap = -(-(4 * tok // experts) // 16) * 16
    w = width // tp
    ny = tp // 2
    r = n * cap
    dma = pltpu.SemaphoreType.DMA
    vmem = pl.BlockSpec(memory_space=pltpu.VMEM)
    anywhere = pl.BlockSpec(memory_space=pl.ANY)
    flops = 6 * r * width * ff
    return pl.pallas_call(
        functools.partial(kernel, n, tp, cap),
        out_shape=jax.ShapeDtypeStruct((tok, w), bf16),
        in_specs=[vmem] * 4 + [anywhere] * 3,
        out_specs=vmem,
        scratch_shapes=[
            pltpu.VMEM((width, ff), bf16),
            pltpu.VMEM((width, ff), bf16),
            pltpu.VMEM((ff, width), bf16),
            pltpu.VMEM((tok, width), bf16),
            pltpu.VMEM((r, w), bf16),
            pltpu.VMEM((r, w), bf16),
            pltpu.VMEM((r, width), bf16),
            pltpu.VMEM((r, ff), bf16),
            pltpu.VMEM((r, width), bf16),
            pltpu.VMEM((r, ny * w), bf16),
            pltpu.VMEM((r, ny * w), bf16),
            pltpu.VMEM((ny - 1, r, w), bf16),
            pltpu.VMEM((r, w), bf16),
            pltpu.VMEM((r, w), bf16),
            pltpu.VMEM((tok, r), bf16),
            pltpu.VMEM((tok, r), bf16),
            dma((3,)),
            dma((n,)), dma((n,)),
            dma((n, ny)), dma((n, ny)),
            dma((n, ny)), dma((n, ny)),
            dma((2, ny)), dma((2, ny)),
            dma((n, ny)), dma((n, ny)),
            dma((n,)), dma((n,)),
        ],
        compiler_params=pltpu.CompilerParams(
            collective_id=0, has_side_effects=True, vmem_limit_bytes=60 * 1024 * 1024),
        cost_estimate=pl.CostEstimate(
            flops=flops, bytes_accessed=6 * width * ff, transcendentals=r * ff),
    )(tokens, norm_gain.reshape(1, -1), expert_ids.T, route_weights.T, w_gate, w_up, w_down)


def solution(mesh):
    in_specs = (
        P("ep", None),
        P(),
        P("ep", None),
        P("ep", None),
        P("ep", None, "tp"),
        P("ep", None, "tp"),
        P("ep", "tp", None),
    )
    out_specs = P("ep", "tp")
    return jax.shard_map(
        per_device, mesh=mesh, in_specs=in_specs, out_specs=out_specs, check_vma=False
    )
```
